512 devices in a mesh: sp: 16 (over z), fs: 4 (over y), tp: 8 (over x, core).
Axes of the slice: x: 4, y: 4, z: 16, core: 2. Of those that a mesh axis runs over, the one named last changes fastest.
Arguments:
- input_layer_rows: bfloat16 [4, 4096, 2048], P('fs', 'sp'), may hold values from -6 to 6
- input_norm_gain: float32 [2048], replicated, may hold values from 0.1 to 1.9
- query_weight_attention: bfloat16 [2048, 1024], P(('sp', 'fs'), 'tp'), may hold values from -0.125 to 0.125
- key_weight_attention: bfloat16 [2048, 1024], P(('sp', 'fs'), 'tp'), may hold values from -0.125 to 0.125
- value_weight_attention: bfloat16 [2048, 1024], P(('sp', 'fs'), 'tp'), may hold values from -0.125 to 0.125
- query_weight_recurrent: bfloat16 [2048, 1024], P(('sp', 'fs'), 'tp'), may hold values from -0.125 to 0.125
- forget_weight_recurrent: bfloat16 [2048, 1024], P(('sp', 'fs'), 'tp'), may hold values from -0.125 to 0.125
- value_weight_recurrent: bfloat16 [2048, 1024], P(('sp', 'fs'), 'tp'), may hold values from -0.125 to 0.125
- gate_weight_recurrent: bfloat16 [2048, 1024], P(('sp', 'fs'), 'tp'), may hold values from -0.125 to 0.125
- output_weight_attention: bfloat16 [2048, 1024], P(('sp', 'fs'), 'tp'), may hold values from -0.125 to 0.125
- emitted_projection_linear_scan: bfloat16 [2048, 1024], P(('sp', 'fs'), 'tp'), may hold values from -0.125 to 0.125
- score_offset: float32 [8], P('tp'), as said below
- attention_norm_gain: float32 [1024], P('tp'), may hold values from 0.1 to 1.9
- recurrence_norm_gain: float32 [1024], P('tp'), may hold values from 0.1 to 1.9
- forget_floor: float32 [1024], P('tp'), may hold values from 0.1 to 0.5
- forget_offset: float32 [1024], P('tp'), as said below
- extra_log_decay: float32 [4, 4096, 1024], P('fs', 'sp', 'tp')
Outputs:
- layer_out: bfloat16 [4, 4096, 2048], P('fs', ('sp', 'tp'))
- row_log_total: float32 [4, 8, 4096], P('fs', 'tp', 'sp')
The draws below stay inside these ranges and needn't reach their ends.
Inputs may be any that keep to these rules, and one draw needn't show every extreme that they name: `score_offset`: each head's offset lies between -ln(4096) - 2 and -ln(4096) + 0.5. `forget_offset`: each channel's offset lies between ln(256) - 3 and ln(4096) + 0.6.
All inputs are finite; a program needn't handle non-finite values.
Results may differ from the reference program's by a relative error of at most 0.015.
Values may be sent and summed in bfloat16 or wider, within the bound.
A program may use at most 64 MiB of HBM per device.

```python
import math
import jax
import jax.numpy as jnp
from jax import lax

HEAD = 128
HEADS = 8
D_HALF = 1024
D = 2048
TOK_DEV = 256
BLOCK = 64
SEQ = 4096
BATCH = 4


def draw_score_offset(key, part):
    center = -math.log(SEQ)
    return jax.random.uniform(key, (HEADS,), jnp.float32, center - 2.0, center + 0.5)


def draw_forget_offset(key, part):
    width = HEADS * HEAD
    first, second, third = jax.random.split(key, 3)
    chooser = jax.random.uniform(first, (width,), jnp.float32)
    slow_value = math.log(SEQ) + jax.random.uniform(second, (width,), jnp.float32, -0.4, 0.6)
    fast_value = math.log(TOK_DEV) - 2.5 + jax.random.uniform(third, (width,), jnp.float32, -0.5, 0.5)
    share = 0.5
    return jnp.where(chooser < share, fast_value, slow_value)


def draw_extra_log_decay(key, part):
    width = HEADS * HEAD
    first, second, third = jax.random.split(key, 3)
    blocks = SEQ // TOK_DEV
    lowest, highest_score = (0.05, 0.4)
    rates = jnp.exp(jax.random.uniform(first, (BATCH, blocks, 1, width), jnp.float32, math.log(lowest), math.log(highest_score))) / SEQ
    constant_component = jnp.broadcast_to(rates, (BATCH, blocks, TOK_DEV, width)).reshape(BATCH, SEQ, width)
    spots = jax.random.randint(second, (BATCH, 3), 0, SEQ)
    stratum_level = jnp.log(jax.random.uniform(third, (BATCH, 3, width), jnp.float32, 0.6, 0.85))
    equality_indicators = (jnp.arange(SEQ)[None, :, None] == spots[:, None, :]).astype(jnp.float32)
    fading_spikes = jnp.einsum('tsk,tkx->tsx', equality_indicators, stratum_level, precision=jax.lax.Precision.HIGHEST)
    return fading_spikes - constant_component


def level_of(rng, extent, shards, smallest, high):
    level, own = 1.0, jax.random.fold_in(rng, 6)
    for axis_at, shards_of in shards:
        heights = jnp.exp(jax.random.uniform(jax.random.fold_in(own, axis_at), (shards_of,), jnp.float32, smallest / len(shards), high / len(shards)))
        level = level * jnp.repeat(heights, extent[axis_at] // shards_of).reshape([-1 if axis == axis_at else 1 for axis in range(len(extent))])
    return level


def normal_values(key, dims, spread, reach, pieces=(), held_as=jnp.bfloat16):
    level = level_of(key, dims, pieces, -0.22, 0.18) if pieces else 1.0
    result = jax.random.normal(key, dims, jnp.float32) * spread * level
    return jnp.minimum(jnp.maximum(result, -reach), reach).astype(held_as)


def setup_inputs(seed: int = 0) -> dict:
    key_of = jax.random.split(jax.random.key(seed), 18)
    input_layer_rows = normal_values(key_of[0], (BATCH, SEQ, D), 1.0, 6.0, ((0, 4), (1, 16)))
    input_norm_gain = jnp.clip(1.0 + 0.18 * jax.random.normal(key_of[1], (D,), jnp.float32), 0.1, 1.9)
    query_weight_attention = normal_values(key_of[2], (D, D_HALF), D ** -0.5, 0.125, ((0, 64), (1, 8)))
    key_weight_attention = normal_values(key_of[3], (D, D_HALF), D ** -0.5, 0.125, ((0, 64), (1, 8)))
    value_weight_attention = normal_values(key_of[4], (D, D_HALF), D ** -0.5, 0.125, ((0, 64), (1, 8)))
    query_weight_recurrent = normal_values(key_of[5], (D, D_HALF), D ** -0.5, 0.125, ((0, 64), (1, 8)))
    forget_weight_recurrent = normal_values(key_of[6], (D, D_HALF), D ** -0.5, 0.125, ((0, 64), (1, 8)))
    value_weight_recurrent = normal_values(key_of[7], (D, D_HALF), D ** -0.5, 0.125, ((0, 64), (1, 8)))
    gate_weight_recurrent = normal_values(key_of[8], (D, D_HALF), D ** -0.5, 0.125, ((0, 64), (1, 8)))
    output_weight_attention = normal_values(key_of[9], (D, D_HALF), D ** -0.5, 0.125, ((0, 64), (1, 8)))
    emitted_projection_linear_scan = normal_values(key_of[10], (D, D_HALF), D ** -0.5, 0.125, ((0, 64), (1, 8)))
    score_offset = draw_score_offset(jax.random.fold_in(key_of[17], 71), 0)
    attention_norm_gain = jnp.clip(1.0 + 0.18 * jax.random.normal(key_of[12], (D_HALF,), jnp.float32), 0.1, 1.9)
    recurrence_norm_gain = jnp.clip(1.0 + 0.18 * jax.random.normal(key_of[13], (D_HALF,), jnp.float32), 0.1, 1.9)
    forget_floor = jnp.clip(0.1 + 0.4 * jax.random.uniform(key_of[14], (D_HALF,), jnp.float32) ** level_of(key_of[14], (D_HALF,), ((0, 8),), -0.2, 0.2), 0.1, 0.5)
    forget_offset = draw_forget_offset(jax.random.fold_in(key_of[17], 71), 0)
    extra_log_decay = draw_extra_log_decay(jax.random.fold_in(key_of[17], 71), 0)
    return {"input_layer_rows": input_layer_rows, "input_norm_gain": input_norm_gain, "query_weight_attention": query_weight_attention, "key_weight_attention": key_weight_attention, "value_weight_attention": value_weight_attention, "query_weight_recurrent": query_weight_recurrent, "forget_weight_recurrent": forget_weight_recurrent, "value_weight_recurrent": value_weight_recurrent, "gate_weight_recurrent": gate_weight_recurrent, "output_weight_attention": output_weight_attention, "emitted_projection_linear_scan": emitted_projection_linear_scan, "score_offset": score_offset, "attention_norm_gain": attention_norm_gain, "recurrence_norm_gain": recurrence_norm_gain, "forget_floor": forget_floor, "forget_offset": forget_offset, "extra_log_decay": extra_log_decay}


epsilon = 1e-06
log_floor = 0.05

def normalize_rows(inputs, gain):
    values = inputs.astype(jnp.float32)
    square_mean = lax.optimization_barrier(jnp.mean(values * values, axis=-1, keepdims=True))
    return values * lax.rsqrt(square_mean + epsilon) * gain

def head_norm(values, gain):
    square_mean = lax.optimization_barrier(jnp.mean(values * values, axis=-1, keepdims=True))
    return values * lax.rsqrt(square_mean + epsilon) * gain

def project(normed, weight):
    return jnp.dot(normed, weight, preferred_element_type=jnp.float32).astype(jnp.bfloat16)

def recurrence_block(memory_matrix, inputs):
    query_slice, decay_part, key_slice, value_slice = inputs
    highest_score = lax.Precision.HIGHEST
    length = decay_part.shape[0]
    running_total = jnp.cumsum(decay_part, axis=0)
    causal = (lax.broadcasted_iota(jnp.int32, (length, length), 0) >= lax.broadcasted_iota(jnp.int32, (length, length), 1))[:, :, None, None]
    relative = jnp.where(causal, running_total[:, None] - running_total[None, :], -jnp.inf)
    pairwise = lax.optimization_barrier(jnp.sum(query_slice[:, None] * key_slice[None, :] * jnp.exp(relative), axis=-1))
    inner_part = jnp.einsum('tsh,shv->thv', pairwise, value_slice, precision=highest_score)
    carried_state = jnp.einsum('fby,bym->fbm', query_slice * jnp.exp(running_total), memory_matrix, precision=highest_score)
    final_total = running_total[-1]
    updated_state = jnp.exp(final_total)[:, :, None] * memory_matrix + jnp.einsum('rxc,rxa->xca', key_slice * jnp.exp(final_total[None] - running_total), value_slice, precision=highest_score)
    return (updated_state, inner_part + carried_state)

def recurrence(query_rows_input, forget_log_value, key_in, value_in):
    seq_len = query_rows_input.shape[0]

    def to_blocks(array_in):
        return array_in.reshape(seq_len // BLOCK, BLOCK, HEADS, HEAD)
    initial = jnp.zeros((HEADS, HEAD, HEAD), jnp.float32)
    unused, outputs = lax.scan(recurrence_block, initial, (to_blocks(query_rows_input), to_blocks(forget_log_value), to_blocks(key_in), to_blocks(value_in)))
    return outputs.reshape(seq_len, HEADS, HEAD)

def stick_attention(queries, keys_all, values_all, shifts):
    outputs = []
    totals = []
    for block_index in range(SEQ // TOK_DEV):
        first = block_index * TOK_DEV
        final = first + TOK_DEV
        scores = jnp.einsum('thd,shd->hts', queries[first:final].astype(jnp.float32), keys_all[:final].astype(jnp.float32)) * HEAD ** (-0.5) + shifts[:, None, None]
        strict = first + lax.broadcasted_iota(jnp.int32, (TOK_DEV, final), 0) > lax.broadcasted_iota(jnp.int32, (TOK_DEV, final), 1)
        logarithmic_retention = jnp.where(strict, jax.nn.log_sigmoid(-scores), 0.0)
        suffix = lax.cumsum(logarithmic_retention, axis=2, reverse=True) - logarithmic_retention
        log_weight = jnp.where(strict, jax.nn.log_sigmoid(scores) + suffix, -jnp.inf)
        weights = jnp.exp(log_weight).astype(jnp.bfloat16)
        outputs.append(jnp.einsum('hts,shd->thd', weights.astype(jnp.float32), values_all[:final].astype(jnp.float32)))
        totals.append(lax.optimization_barrier(jnp.sum(logarithmic_retention, axis=2)))
    return (jnp.concatenate(outputs, axis=0), jnp.concatenate(totals, axis=1))

def reference(input_layer_rows, input_norm_gain, query_weight_attention, key_weight_attention, value_weight_attention, query_weight_recurrent, forget_weight_recurrent, value_weight_recurrent, gate_weight_recurrent, output_weight_attention, emitted_projection_linear_scan, score_offset, attention_norm_gain, recurrence_norm_gain, forget_floor, forget_offset, extra_log_decay):
    layer_rows = []
    log_rows = []
    for batch_position in range(BATCH):
        normed = normalize_rows(input_layer_rows[batch_position], input_norm_gain).astype(jnp.bfloat16)
        query_a = project(normed, query_weight_attention).reshape(SEQ, HEADS, HEAD)
        key_a = project(normed, key_weight_attention).reshape(SEQ, HEADS, HEAD)
        value_a = project(normed, value_weight_attention).reshape(SEQ, HEADS, HEAD)
        query_b = project(normed, query_weight_recurrent)
        forget_b = project(normed, forget_weight_recurrent)
        input_b = project(normed, value_weight_recurrent)
        gate_b = project(normed, gate_weight_recurrent)
        attended, keep_total = stick_attention(query_a, key_a, value_a, score_offset)
        log_rows.append(jnp.log(jnp.maximum(-jnp.expm1(keep_total), log_floor)))
        mixed_a = head_norm(attended, attention_norm_gain.reshape(HEADS, HEAD)).reshape(SEQ, D_HALF).astype(jnp.bfloat16)
        forget_logits = forget_b.astype(jnp.float32) + forget_offset
        forget_log_value = jnp.logaddexp(jnp.log(forget_floor), jnp.log1p(-forget_floor) + jax.nn.log_sigmoid(forget_logits)) + extra_log_decay[batch_position]
        key_in = (1.0 - forget_floor) * jax.nn.sigmoid(-forget_logits)
        query_rows_input = jax.nn.silu(query_b.astype(jnp.float32))
        value_in = input_b.astype(jnp.float32)
        recurrent = recurrence(query_rows_input.reshape(SEQ, HEADS, HEAD), forget_log_value.reshape(SEQ, HEADS, HEAD), key_in.reshape(SEQ, HEADS, HEAD), value_in.reshape(SEQ, HEADS, HEAD))
        gated_out = head_norm(recurrent, recurrence_norm_gain.reshape(HEADS, HEAD)) * jax.nn.silu(gate_b.astype(jnp.float32).reshape(SEQ, HEADS, HEAD))
        mixed_b = gated_out.reshape(SEQ, D_HALF).astype(jnp.bfloat16)
        summed = jnp.dot(mixed_a, output_weight_attention.T, preferred_element_type=jnp.float32) + jnp.dot(mixed_b, emitted_projection_linear_scan.T, preferred_element_type=jnp.float32)
        layer_rows.append(summed.astype(jnp.bfloat16))
    return (jnp.stack(layer_rows), jnp.stack(log_rows))
```

```python
import functools

import jax
import jax.numpy as jnp
from jax import lax
from jax.experimental import pallas as pl
from jax.experimental.pallas import tpu as pltpu
from jax.sharding import PartitionSpec as P

HEAD = 128
SUB = 16
EPS = 1e-06
FLOOR = 0.05
CHUNKS = 3
MESH = pl.DeviceIdType.MESH
F32 = jnp.float32
BF16 = jnp.bfloat16


def mm(a, b, ca=1, cb=0):
    return lax.dot_general(a, b, (((ca,), (cb,)), ((), ())), preferred_element_type=F32)


def split_mm(ones, a, terms):
    total = None
    for _ in range(terms):
        part = a.astype(BF16)
        a = a - part.astype(F32)
        term = mm(ones, part)
        total = term if total is None else total + term
    return total


def iotas(rows, cols):
    return (
        lax.broadcasted_iota(jnp.int32, (rows, cols), 0),
        lax.broadcasted_iota(jnp.int32, (rows, cols), 1),
    )


def sigmoid(v):
    return 1.0 / (1.0 + jnp.exp(-v))


def head_norm(v, gain):
    return v * lax.rsqrt(jnp.mean(v * v, axis=-1, keepdims=True) + EPS) * gain


def kernel(n, m, tp, *refs):
    (
        x_ref, gain_ref, qa_ref, ka_ref, va_ref, qb_ref, fb_ref, ib_ref, gb_ref, oa_ref, ob_ref,
        off_ref, again_ref, rgain_ref, floor_ref, foff_ref, extra_ref,
        out_ref, total_ref,
        xbuf, nbuf, ebuf, w0, w1, kvb, stb, qatt, accn, accf, keepn, keepf, incn, incf, decn, tri,
        qpad, rpad, kpad, vpad, recl, qdec, gate, mix, pbuf, prt, comb, xrecv,
        lsem, zus, zds, zur, zdr, yrs, yls, rrs, rls, lup, rdn, ldn, rup, l2, r2,
        bs, br, kus, kds, kur, kdr, ps, pr, xs, xr,
    ) = refs
    z, y, t8 = lax.axis_index("sp"), lax.axis_index("fs"), lax.axis_index("tp")
    tok, depth = xbuf.shape
    nup, ndn = n // 2, (n - 1) // 2
    half = n // 2
    zu, zd = lax.rem(z + 1, n), lax.rem(z + n - 1, n)
    yr, yl = lax.rem(y + 1, m), lax.rem(y + m - 1, m)
    nx = tp // 2
    core, xi = lax.rem(t8, 2), lax.div(t8, 2)
    partner = t8 + 1 - 2 * core

    local = [
        pltpu.make_async_copy(src, w0.at[z, y, :, pl.ds(k * HEAD, HEAD)], lsem.at[k])
        for k, src in enumerate((ka_ref, va_ref, qa_ref, fb_ref, ib_ref))
    ] + [
        pltpu.make_async_copy(src, w1.at[z, y, :, pl.ds(k * HEAD, HEAD)], lsem.at[5 + k])
        for k, src in enumerate((qb_ref, gb_ref, oa_ref, ob_ref))
    ]
    xcopy = pltpu.make_async_copy(x_ref.at[0], xbuf, lsem.at[9])
    ecopy = pltpu.make_async_copy(extra_ref.at[0], ebuf, lsem.at[10])
    for copy in local:
        copy.start()
    xcopy.start()
    ecopy.start()

    barrier = pltpu.get_barrier_semaphore()
    peers = [{"sp": zu}, {"sp": zd}]
    if m > 1:
        peers += [{"fs": yr}, {"fs": yl}]
    if tp > 1:
        peers += [{"tp": partner}]
        peers += [{"tp": lax.rem(xi + k, nx) * 2 + core} for k in range(1, nx)]
    for peer in peers:
        pl.semaphore_signal(barrier, inc=1, device_id=peer, device_id_type=MESH)
    for copy in local:
        copy.wait()
    pl.semaphore_wait(barrier, len(peers))

    def rc(src, dst, ssem, rsem, peer):
        return pltpu.make_async_remote_copy(
            src_ref=src, dst_ref=dst, send_sem=ssem, recv_sem=rsem, device_id=peer, device_id_type=MESH
        )

    ws = (w0, w1)

    def zup(g, t, block):
        ref = ws[g].at[block, y]
        return rc(ref, ref, zus.at[g], zur.at[g, t], {"sp": zu})

    def zdn(g, t, block):
        ref = ws[g].at[block, y]
        return rc(ref, ref, zds.at[g], zdr.at[g, t], {"sp": zd})

    def to_right(block, rsem):
        ref = w0.at[block, y]
        return rc(ref, ref, yrs, rsem, {"fs": yr})

    def to_left(block, rsem):
        ref = w0.at[block, y]
        return rc(ref, ref, yls, rsem, {"fs": yl})

    def relay_right(block):
        ref = w0.at[block, yl]
        return rc(ref, ref, rrs, l2, {"fs": yr})

    def relay_left(block):
        ref = w0.at[block, yr]
        return rc(ref, ref, rls, r2, {"fs": yl})

    def from_left(block, sem):
        ref = w0.at[block, yl]
        return rc(ref, ref, yrs, sem, {"fs": yr})

    def from_right(block, sem):
        ref = w0.at[block, yr]
        return rc(ref, ref, yls, sem, {"fs": yl})

    for g in (0, 1):
        zup(g, 0, z).start()
        if ndn:
            zdn(g, 0, z).start()
        if g == 0 and m > 1:
            to_right(z, lup.at[0]).start()
            to_left(z, rup).start()

    rows, cols = iotas(tok, tok)
    tri[...] = jnp.where(rows > cols, 1.0, 0.0).astype(BF16)
    xcopy.wait()

    @pl.loop(0, tok // 32)
    def _(r):
        at = pl.ds(pl.multiple_of(r * 32, 32), 32)
        v = xbuf[at, :].astype(F32)
        v = v * lax.rsqrt(jnp.mean(v * v, axis=-1, keepdims=True) + EPS)
        nbuf[at, :] = (v * gain_ref[...].reshape(1, depth)).astype(BF16)

    @pl.loop(1, nup + 1)
    def _(t):
        up, dn = lax.rem(z - t + n, n), lax.rem(z + t, n)
        zup(0, t - 1, up).wait_recv()

        @pl.when(t < nup)
        def _():
            zup(0, t, up).start()

        if m > 1:
            to_right(up, lup.at[t]).start()
            to_left(up, rup).start()

        if ndn:
            @pl.when(t <= ndn)
            def _():
                zdn(0, t - 1, dn).wait_recv()

                @pl.when(t < ndn)
                def _():
                    zdn(0, t, dn).start()

                if m > 1:
                    to_right(dn, ldn).start()
                    to_left(dn, rdn.at[t - 1]).start()

        zup(1, t - 1, up).wait_recv()

        @pl.when(t < nup)
        def _():
            zup(1, t, up).start()

        if ndn:
            @pl.when(t <= ndn)
            def _():
                zdn(1, t - 1, dn).wait_recv()

                @pl.when(t < ndn)
                def _():
                    zdn(1, t, dn).start()

        if m > 1:
            before = lax.rem(z - t + 1 + n, n)
            from_left(before, lup.at[t - 1]).wait_recv()
            relay_right(before).start()
            if ndn:
                @pl.when(t >= 2)
                def _():
                    late = lax.rem(z + t - 1, n)
                    from_right(late, rdn.at[t - 2]).wait_recv()
                    relay_left(late).start()

    last = lax.rem(z - nup + n, n)
    lo, hi = pl.ds(0, half), pl.ds(half, n - half)

    def bulk(k, part, src, peer):
        ref = w1.at[part, src]
        return rc(ref, ref, bs.at[k], br.at[k], peer)

    if m > 1:
        from_left(last, lup.at[nup]).wait_recv()
        relay_right(last).start()
        bulk(0, lo, y, {"fs": yr}).start()
        bulk(1, hi, y, {"fs": yl}).start()
        bulk(2, hi, y, {"fs": yr}).start()
        bulk(3, lo, y, {"fs": yl}).start()

        def waited(count, sem):
            ref = w0.at[pl.ds(0, count), 0]
            pltpu.make_async_copy(ref, ref, sem).wait()

        waited(nup + 1, rup)
        waited(nup + 1, l2)
        if ndn:
            waited(ndn, ldn)
            waited(ndn, r2)

    p0 = mm(nbuf[...], w0[...].reshape(depth, 5 * HEAD)).astype(BF16)
    kvb[z] = p0[:, : 2 * HEAD]
    qatt[...] = p0[:, 2 * HEAD : 3 * HEAD]
    floor = floor_ref[...].reshape(1, HEAD)
    u = p0[:, 3 * HEAD : 4 * HEAD].astype(F32) + foff_ref[...].reshape(1, HEAD)
    key = (1.0 - floor) * sigmoid(-u)
    ecopy.wait()
    step = jnp.log(1.0 - key) + ebuf[...]
    run = split_mm(jnp.where(rows >= cols, 1.0, 0.0).astype(BF16), step, 3)
    val = p0[:, 4 * HEAD : 5 * HEAD]
    end = run[tok - 1 :, :]
    state = mm(val, (key * jnp.exp(end - run)).astype(BF16), 0, 0)
    stb[z, :HEAD, :] = state.astype(BF16)
    stb[z, HEAD:, :] = jnp.broadcast_to(jnp.exp(end), (SUB, HEAD)).astype(BF16)
    zero = jnp.zeros((SUB, HEAD), F32)
    rpad[:SUB, :] = zero
    kpad[:SUB, :] = zero
    vpad[:SUB, :] = zero
    rpad[SUB:, :] = run
    kpad[SUB:, :] = key
    vpad[SUB:, :] = val.astype(F32)

    th = tok // 2

    def pieces(block):
        return (kvb.at[block, pl.ds(0, th)], kvb.at[block, pl.ds(th, th)], stb.at[block])

    def kup(t, block):
        return [
            rc(ref, ref, kus.at[t, c], kur.at[t, c], {"sp": zu}) for c, ref in enumerate(pieces(block))
        ]

    def kdn(t, block):
        return [
            rc(ref, ref, kds.at[t, c], kdr.at[t, c], {"sp": zd}) for c, ref in enumerate(pieces(block))
        ]

    @pl.when(z < n - 1)
    def _():
        for copy in kup(0, z):
            copy.start()

    if ndn:
        @pl.when(z < ndn)
        def _():
            for copy in kdn(0, z):
                copy.start()

    shift = off_ref[0]

    def attend(block, masked):
        s = mm(qatt[...], kvb[block, :, :HEAD], 1, 1) * HEAD ** (-0.5) + shift
        soft = jnp.maximum(s, 0.0) + jnp.log(1.0 + jnp.exp(-jnp.abs(s)))
        keep = -soft
        if masked:
            keep = jnp.where(rows > cols, keep, 0.0)
        big = keep.astype(BF16)
        small = (keep - big.astype(F32)).astype(BF16)
        suffix = mm(big, tri[...]) + mm(small, tri[...])
        w = jnp.exp(s - soft + suffix)
        if masked:
            w = jnp.where(rows > cols, w, 0.0)
        o = mm(w.astype(BF16), kvb[block, :, HEAD:])
        return o, jnp.broadcast_to(suffix[:, :1] + keep[:, :1], (tok, HEAD))

    o, gone = attend(z, True)
    accn[...] = o
    keepn[...] = gone
    accf[...] = jnp.zeros_like(accf)
    keepf[...] = jnp.zeros_like(keepf)
    incn[...] = jnp.zeros_like(incn)
    incf[...] = jnp.zeros_like(incf)
    decn[...] = jnp.ones_like(decn)

    def local_recurrence():
        pb = mm(nbuf[...], w1[:, :, :, : 2 * HEAD].reshape(depth, 2 * HEAD)).astype(BF16)
        q = pb[:, :HEAD].astype(F32)
        q = q * sigmoid(q)
        g = pb[:, HEAD:].astype(F32)
        gate[...] = g * sigmoid(g)
        r = rpad[SUB:, :]
        qdec[...] = (q * jnp.exp(r)).astype(BF16)
        ones = jnp.ones((HEAD, HEAD), BF16)
        place = lax.rem(lax.broadcasted_iota(jnp.int32, (tok, HEAD), 0), SUB)
        acc = jnp.zeros((tok, HEAD), F32)
        for d in range(SUB):
            at = pl.ds(SUB - d, tok)
            a = q * kpad[at, :] * jnp.exp(r - rpad[at, :])
            a = jnp.where(place >= d, a, 0.0)
            acc += mm(a.astype(BF16), ones) * vpad[at, :]
        recl[...] = acc
        qpad[...] = q
        for i in range(1, tok // SUB):
            b = i * SUB
            start = rpad[SUB + b - 1 : SUB + b, :]
            rt = rpad[SUB + b : 2 * SUB + b, :] - start
            top = jnp.maximum(jnp.max(rt, axis=0, keepdims=True), 0.0)
            qh = (qpad[b : b + SUB, :] * jnp.exp(rt - top)).astype(BF16)
            kh = kpad[SUB : SUB + b, :] * jnp.exp(start + top - rpad[SUB : SUB + b, :])
            pair = mm(qh, kh.astype(BF16), 1, 1).astype(BF16)
            recl[b : b + SUB, :] += mm(pair, vpad[SUB : SUB + b, :].astype(BF16))

    relay_at = min(3, max(nup - 1, 1))
    use_at = max(nup - 1, 1)

    @pl.loop(1, nup + 1)
    def _(t):
        up, dn = z - t, lax.rem(z + t, n)
        up0 = jnp.maximum(up, 0)
        for c in range(CHUNKS):
            @pl.when(z >= t)
            def _():
                kup(t - 1, up0)[c].wait_recv()

                @pl.when(jnp.logical_and(t < nup, z < n - 1))
                def _():
                    kup(t, up0)[c].start()

            if ndn:
                @pl.when(jnp.logical_and(t <= ndn, dn < ndn))
                def _():
                    kdn(t - 1, dn)[c].wait_recv()

                    @pl.when(t < ndn)
                    def _():
                        kdn(t, dn)[c].start()

        if m > 1:
            @pl.when(t == relay_at)
            def _():
                bulk(0, lo, yl, {"fs": yr}).wait_recv()
                bulk(4, lo, yl, {"fs": yr}).start()
                bulk(1, hi, yr, {"fs": yl}).wait_recv()
                bulk(5, hi, yr, {"fs": yl}).start()

        @pl.when(z >= t)
        def _():
            o, gone = attend(up0, False)
            accn[...] += jnp.exp(keepn[...]) * o
            keepn[...] += gone
            incn[...] += decn[:1, :] * stb[up0, :HEAD, :].astype(F32)
            decn[...] *= stb[up0, HEAD : HEAD + 8, :].astype(F32)

        if ndn:
            @pl.when(jnp.logical_and(t <= ndn, z + t >= n))
            def _():
                o, gone = attend(dn, False)
                accf[...] = o + jnp.exp(gone) * accf[...]
                keepf[...] += gone
                decay = stb[dn, HEAD : HEAD + 8, :].astype(F32)
                incf[...] = decay[:1, :] * incf[...] + stb[dn, :HEAD, :].astype(F32)

        @pl.when(t == use_at)
        def _():
            if m > 1:
                y2 = lax.rem(y + 2, m)
                bulk(2, hi, yl, {"fs": yr}).wait_recv()
                bulk(3, lo, yr, {"fs": yl}).wait_recv()
                bulk(4, lo, y2, {"fs": yr}).wait_recv()
                bulk(5, hi, y2, {"fs": yl}).wait_recv()
            local_recurrence()

    attended = accn[...] + jnp.exp(keepn[...]) * accf[...]
    keep = keepn[...] + keepf[...]
    logs = jnp.log(jnp.maximum(1.0 - jnp.exp(keep), FLOOR))
    total_ref[...] = jnp.transpose(logs)[:1, :].reshape(1, 1, tok)
    entering = incn[...] + decn[:1, :] * incf[...]
    recurrent = recl[...] + mm(qdec[...], entering.astype(BF16), 1, 1)
    mix[:, :HEAD] = head_norm(attended, again_ref[...].reshape(1, HEAD)).astype(BF16)
    mix[:, HEAD:] = (
        head_norm(recurrent, rgain_ref[...].reshape(1, HEAD)) * gate[...]
    ).astype(BF16)

    width = depth // 2

    def product(h):
        weight = w1[pl.ds(h * half, half), :, :, 2 * HEAD :].reshape(width, 2 * HEAD)
        return mm(mix[...], weight, 1, 1)

    if tp == 1:
        for h in range(2):
            out_ref[0, :, h * width : (h + 1) * width] = product(h).astype(BF16)
    else:
        def to_partner(h):
            return rc(pbuf.at[h, :, 1 - core], prt.at[h], ps.at[h], pr.at[h], {"tp": partner})

        def to_chip(h, k):
            x2 = lax.rem(xi + k, nx)
            return rc(
                comb.at[h, x2], xrecv.at[h, k - 1], xs.at[h, k - 1], xr.at[h, k - 1],
                {"tp": x2 * 2 + core},
            )

        for h in range(2):
            pbuf[h] = product(h).astype(BF16).reshape(nx, 2, tok // tp, width)
            to_partner(h).start()
        for h in range(2):
            to_partner(h).wait_recv()
            both = pbuf[h, :, core].astype(F32) + prt[h].astype(F32)
            comb[h] = both.astype(BF16)
            for k in range(1, nx):
                to_chip(h, k).start()
        for h in range(2):
            whole = comb[h, xi].astype(F32)
            for k in range(1, nx):
                to_chip(h, k).wait_recv()
                whole += xrecv[h, k - 1].astype(F32)
            out_ref[0, :, h * width : (h + 1) * width] = whole.astype(BF16)

    def sent(ref, sem):
        pltpu.make_async_copy(ref, ref, sem).wait()

    for g in (0, 1):
        sent(ws[g].at[pl.ds(0, nup), 0], zus.at[g])
        if ndn:
            sent(ws[g].at[pl.ds(0, ndn), 0], zds.at[g])
    if m > 1:
        sent(w0.at[pl.ds(0, n), 0], yrs)
        sent(w0.at[pl.ds(0, n), 0], yls)
        sent(w0.at[pl.ds(0, nup + 1), 0], rrs)
        if ndn:
            sent(w0.at[pl.ds(0, ndn), 0], rls)
        for k, part, peer in (
            (0, lo, yr), (1, hi, yl), (2, hi, yr), (3, lo, yl), (4, lo, yr), (5, hi, yl),
        ):
            bulk(k, part, y, {"fs": peer}).wait_send()

    @pl.loop(0, nup)
    def _(t):
        up, dn = jnp.maximum(z - t, 0), lax.rem(z + t, n)

        @pl.when(jnp.logical_and(z >= t, z < n - 1))
        def _():
            for copy in kup(t, up):
                copy.wait_send()

        if ndn:
            @pl.when(jnp.logical_and(t < ndn, dn < ndn))
            def _():
                for copy in kdn(t, dn):
                    copy.wait_send()

    if tp > 1:
        for h in range(2):
            to_partner(h).wait_send()
            for k in range(1, nx):
                to_chip(h, k).wait_send()


def on_device(n, m, tp, *args):
    tok, depth = args[0].shape[1:]
    nx = max(tp // 2, 1)
    rows = tok // tp
    nup, ndn = n // 2, max((n - 1) // 2, 1)
    vm, dma = pltpu.VMEM, pltpu.SemaphoreType.DMA
    whole = pl.BlockSpec(memory_space=pltpu.VMEM)
    there = pl.BlockSpec(memory_space=pl.ANY)
    scalar = pl.BlockSpec(memory_space=pltpu.SMEM)
    wide = (nx, 2, rows, depth // 2) if tp > 1 else (1, 1, 16, 128)
    part = (nx, rows, depth // 2) if tp > 1 else (1, 16, 128)
    return pl.pallas_call(
        functools.partial(kernel, n, m, tp),
        out_shape=(
            jax.ShapeDtypeStruct((1, rows, depth), BF16),
            jax.ShapeDtypeStruct((1, 1, tok), F32),
        ),
        in_specs=[there, whole] + [there] * 9 + [scalar] + [whole] * 4 + [there],
        out_specs=(whole, whole),
        scratch_shapes=[
            vm((tok, depth), BF16),
            vm((tok, depth), BF16),
            vm((tok, HEAD), F32),
            vm((n, m, 32, 5 * HEAD), BF16),
            vm((n, m, 32, 4 * HEAD), BF16),
            vm((n, tok, 2 * HEAD), BF16),
            vm((n, HEAD + SUB, HEAD), BF16),
            vm((tok, HEAD), BF16),
            vm((tok, HEAD), F32),
            vm((tok, HEAD), F32),
            vm((tok, HEAD), F32),
            vm((tok, HEAD), F32),
            vm((HEAD, HEAD), F32),
            vm((HEAD, HEAD), F32),
            vm((8, HEAD), F32),
            vm((tok, tok), BF16),
            vm((tok, HEAD), F32),
            vm((SUB + tok, HEAD), F32),
            vm((SUB + tok, HEAD), F32),
            vm((SUB + tok, HEAD), F32),
            vm((tok, HEAD), F32),
            vm((tok, HEAD), BF16),
            vm((tok, HEAD), F32),
            vm((tok, 2 * HEAD), BF16),
            vm((2, *wide), BF16),
            vm((2, *part), BF16),
            vm((2, *part), BF16),
            vm((2, max(nx - 1, 1), *part[1:]), BF16),
            dma((11,)),
            dma((2,)),
            dma((2,)),
            dma((2, nup)),
            dma((2, ndn)),
            dma,
            dma,
            dma,
            dma,
            dma((nup + 1,)),
            dma((ndn,)),
            dma,
            dma,
            dma,
            dma,
            dma((6,)),
            dma((6,)),
            dma((nup, CHUNKS)),
            dma((ndn, CHUNKS)),
            dma((nup, CHUNKS)),
            dma((ndn, CHUNKS)),
            dma((2,)),
            dma((2,)),
            dma((2, max(nx - 1, 1))),
            dma((2, max(nx - 1, 1))),
        ],
        compiler_params=pltpu.CompilerParams(
            collective_id=0, has_side_effects=True, vmem_limit_bytes=60 * 1024 * 1024
        ),
        name="layer",
    )(*args)


def solution(mesh):
    size = mesh.shape
    weight = P(("sp", "fs"), "tp")
    return jax.shard_map(
        functools.partial(on_device, size["sp"], size["fs"], size["tp"]),
        mesh=mesh,
        in_specs=(P("fs", "sp", None), P(), *[weight] * 9, *[P("tp")] * 5, P("fs", "sp", "tp")),
        out_specs=(P("fs", ("sp", "tp"), None), P("fs", "tp", "sp")),
        check_vma=False,
    )
```
